512 devices in a mesh: grp: 2 (over y), fs: 16 (over z), tp: 16 (over x, core).
Axes of the slice: x: 8, y: 2, z: 16, core: 2. Of those that a mesh axis runs over, the one named last changes fastest.
The devices are a block of a 8x16x16 slice.
Arguments:
- tokens: bfloat16 [4096, 2048], P(('grp', 'fs')), parts along dimension 0, may hold values from -12 to 12, as said below
- mix_heads: bfloat16 [4096, 2048], P(('grp', 'fs'), 'tp'), parts along dimension 0, may hold values from -6 to 6
- norm_first: float32 [2048], replicated, may hold values from 0.1 to 1.9
- gate_first: bfloat16 [2048, 5632], P('fs', 'tp'), may hold values from -0.125 to 0.125
- up_first: bfloat16 [2048, 5632], P('fs', 'tp'), may hold values from -0.125 to 0.125
- down_first: bfloat16 [5632, 2048], P('tp', 'fs'), may hold values from -0.078125 to 0.078125
- out_weight: bfloat16 [2048, 2048], P('tp', 'fs'), may hold values from -0.125 to 0.125
- norm_second: float32 [2048], replicated, may hold values from 0.1 to 1.9
- gate_second: bfloat16 [2048, 5632], P('fs', 'tp'), may hold values from -0.125 to 0.125
- up_second: bfloat16 [2048, 5632], P('fs', 'tp'), may hold values from -0.125 to 0.125
- down_second: bfloat16 [5632, 2048], P('tp', 'fs'), may hold values from -0.078125 to 0.078125
Outputs:
- layer_out: bfloat16 [4096, 2048], P(('grp', 'fs')), parts along dimension 0
The draws below stay inside these ranges and needn't reach their ends.
There are 2 independent parts, one for each index of `grp`. The reference program is written for one: setup_inputs(seed, part) draws one part's arguments, and reference() takes and returns one part's arrays. A program takes and returns all parts, laid end to end along the dimension named above; an argument that names none is the same for every part. Nothing has to cross between parts.
Inputs may be any that keep to these rules, and one draw needn't show every extreme that they name: Each row of tokens carries a scale of its own.
All inputs are finite; a program needn't handle non-finite values.
Results may differ from the reference program's by a relative error of at most 0.014.
Values may be sent and summed in bfloat16 or wider, within the bound.
A program may use at most 64 MiB of HBM per device.

```python
import math
import jax
import jax.numpy as jnp
from jax import lax

D = 2048
FF = 5632
MIX = 2048
TOKENS = 2048
N_TP = 16


def draw_tokens(key, part):
    subkeys = jax.random.split(key, 3)
    base_values = jax.random.normal(subkeys[0], (TOKENS, D), jnp.float32)
    row_scale = jnp.exp(jax.random.uniform(subkeys[1], (TOKENS, 1), jnp.float32, math.log(0.4), math.log(2.5)))
    values = base_values * row_scale
    return jnp.clip(values, -12.0, 12.0).astype(jnp.bfloat16)


def levels(key, dims, cuts, smallest, largest):
    loudness, own = 1.0, jax.random.fold_in(key, 6)
    for position, shards_of in cuts:
        steps = jnp.exp(jax.random.uniform(jax.random.fold_in(own, position), (shards_of,), jnp.float32, smallest / len(cuts), largest / len(cuts)))
        loudness = loudness * jnp.repeat(steps, dims[position] // shards_of).reshape([-1 if axis == position else 1 for axis in range(len(dims))])
    return loudness


def centred(stream_key, dims, deviation, most, cuts=(), dtype=jnp.bfloat16):
    level = levels(stream_key, dims, cuts, -0.22, 0.18) if cuts else 1.0
    entries = jax.random.normal(stream_key, dims, jnp.float32) * deviation * level
    return jnp.minimum(jnp.maximum(entries, -most), most).astype(dtype)


def setup_inputs(seed: int = 0, part: int = 0) -> dict:
    keys = jax.random.split(jax.random.key(seed), 12)
    part_keys = jax.random.split(jax.random.fold_in(keys[11], part), 12)
    return {
        "tokens": draw_tokens(jax.random.fold_in(jax.random.fold_in(keys[11], part), 71), part),
        "mix_heads": centred(part_keys[1], (TOKENS, MIX), 1.0, 6.0, ((0, 16), (1, 16))),
        "norm_first": jnp.clip(1.0 + 0.18 * jax.random.normal(keys[2], (D,), jnp.float32), 0.1, 1.9),
        "gate_first": centred(keys[3], (D, FF), D ** -0.5, 0.125, ((0, 16), (1, 16))),
        "up_first": centred(keys[4], (D, FF), D ** -0.5, 0.125, ((0, 16), (1, 16))),
        "down_first": centred(keys[5], (FF, D), FF ** -0.5, 0.078125, ((0, 16), (1, 16))),
        "out_weight": centred(keys[6], (MIX, D), MIX ** -0.5, 0.125, ((0, 16), (1, 16))),
        "norm_second": jnp.clip(1.0 + 0.18 * jax.random.normal(keys[7], (D,), jnp.float32), 0.1, 1.9),
        "gate_second": centred(keys[8], (D, FF), D ** -0.5, 0.125, ((0, 16), (1, 16))),
        "up_second": centred(keys[9], (D, FF), D ** -0.5, 0.125, ((0, 16), (1, 16))),
        "down_second": centred(keys[10], (FF, D), FF ** -0.5, 0.078125, ((0, 16), (1, 16))),
    }


EPS = 0.1

def norm_rows(row_block, gain_vector):
    widened = row_block.astype(jnp.float32)
    scaled = widened * lax.rsqrt(lax.optimization_barrier(jnp.mean(widened * widened, axis=-1, keepdims=True)) + EPS)
    return (scaled * gain_vector.astype(jnp.float32)).astype(jnp.bfloat16)

def branch_terms(normed, gate_weight, value_weight, down_weight, added_term):
    block_width = FF // N_TP

    def block_term(index):
        first_col = (index * block_width).astype(jnp.int32)
        gates = jnp.dot(normed, lax.dynamic_slice_in_dim(gate_weight, first_col, block_width, 1), preferred_element_type=jnp.float32)
        values = jnp.dot(normed, lax.dynamic_slice_in_dim(value_weight, first_col, block_width, 1), preferred_element_type=jnp.float32)
        hidden = (jax.nn.silu(gates) * values).astype(jnp.bfloat16)
        partial_value = 0.5 * jnp.dot(hidden, lax.dynamic_slice_in_dim(down_weight, first_col, block_width, 0), preferred_element_type=jnp.float32)
        return partial_value + added_term(index)

    def accumulate(index, total):
        rounded = lax.optimization_barrier(block_term(index).astype(jnp.bfloat16))
        return total + rounded.astype(jnp.float32)
    start_total = jnp.zeros((normed.shape[0], down_weight.shape[1]), jnp.float32)
    return lax.fori_loop(0, N_TP, accumulate, start_total)

def reference(tokens, mix_heads, norm_first, gate_first, up_first, down_first, out_weight, norm_second, gate_second, up_second, down_second):
    head_width = MIX // N_TP

    def head_term(index):
        first_col = (index * head_width).astype(jnp.int32)
        heads = lax.dynamic_slice_in_dim(mix_heads, first_col, head_width, 1)
        weight_rows = lax.dynamic_slice_in_dim(out_weight, first_col, head_width, 0)
        return jnp.dot(heads, weight_rows, preferred_element_type=jnp.float32)

    def no_term(index):
        return jnp.zeros((tokens.shape[0], tokens.shape[1]), jnp.float32)
    normed_one = norm_rows(tokens, norm_first)
    mixed_sum = branch_terms(normed_one, gate_first, up_first, down_first, head_term)
    resid_two = tokens.astype(jnp.float32) + mixed_sum
    normed_two = norm_rows(resid_two, norm_second)
    ffn_sum = branch_terms(normed_two, gate_second, up_second, down_second, no_term)
    return (resid_two + ffn_sum).astype(jnp.bfloat16)
```

```python
import functools

import jax
import jax.numpy as jnp
from jax import lax
from jax.experimental import pallas as pl
from jax.experimental.pallas import tpu as pltpu
from jax.sharding import PartitionSpec as P

EPS = 0.1
PAIRED = False
RIGHT, LEFT = 0, 1
FIRST, SECOND = (0, 1, 2), (3, 4, 5)
OFFSETS = (0, 0, 1, 8, 8, 10)
SLOTS = 19
SUM_AFTER = 3
JOIN_AFTER = 3
GROUPS = ((0, 9), (9, 13), (13, 16))


def steps_positions(step):
    if step == 0:
        return (0,)
    return (15,) if step == 8 else (2 * step - 1, 2 * step)


def nt(a, b):
    return lax.dot_general(a, b, (((1,), (1,)), ((), ())), preferred_element_type=jnp.float32)


def body(
    tok, mix, gain1, gain2, g1, u1, d1, ow, g2, u2, d2,
    out,
    w0, w1, w2, w3, w4, w5, xf, x1, acc, hid, t1, r1, t2, r2, nrm, x2, fin, done, resid,
    wsem, ssem, rsem, ysend, yrecv, xsend, xrecv,
):
    W = (w0, w1, w2, w3, w4, w5)
    z, tp, gr = lax.axis_index("fs"), lax.axis_index("tp"), lax.axis_index("grp")
    nz, ntp = lax.axis_size("fs"), lax.axis_size("tp")
    right, left = lax.rem(z + 1, nz), lax.rem(z + nz - 1, nz)
    parity = lax.rem(gr, 2)
    mate = gr + 1 - 2 * parity
    share = tok.shape[0] // ntp
    wide = tok.shape[1] // nz
    hidden_rows = g1.shape[1]

    def block_of(pos):
        if pos == 0:
            return z
        if pos == 15:
            return lax.rem(z + 8, nz)
        step = (pos + 1) // 2
        return lax.rem(z + nz - step, nz) if pos % 2 else lax.rem(z + step, nz)

    def cut(c):
        rows = W[c].shape[1]
        lent = rows // 3 // 16 * 16
        if not PAIRED:
            return 0, rows, 0, 0
        return pl.multiple_of(parity * lent, 16), rows - lent, pl.multiple_of((1 - parity) * (rows - lent), 16), lent

    barrier = pltpu.get_barrier_semaphore()
    pl.semaphore_signal(barrier, device_id={"fs": right}, device_id_type=pl.DeviceIdType.MESH)
    pl.semaphore_signal(barrier, device_id={"fs": left}, device_id_type=pl.DeviceIdType.MESH)
    for d in range(1, 16):
        pl.semaphore_signal(barrier, device_id={"tp": lax.rem(tp + d, ntp)}, device_id_type=pl.DeviceIdType.MESH)
    if PAIRED:
        pl.semaphore_signal(barrier, device_id={"grp": mate}, device_id_type=pl.DeviceIdType.MESH)

    loads = [
        pltpu.make_async_copy(d1, w2.at[0, 0:hidden_rows], wsem.at[0]),
        pltpu.make_async_copy(ow, w2.at[0, hidden_rows : w2.shape[1]], wsem.at[1]),
        pltpu.make_async_copy(d2, w5.at[0], wsem.at[2]),
    ]
    for load in loads:
        load.start()
    w0[0] = g1[...].T
    w1[0] = u1[...].T
    w3[0] = g2[...].T
    w4[0] = u2[...].T
    for load in loads:
        load.wait()
    pl.semaphore_wait(barrier, 18 if PAIRED else 17)

    sends = []

    def ring_copy(c, way, step):
        start, keep, _, _ = cut(c)
        if step == 7:
            half = keep // 32 * 16
            src = 13 if way == RIGHT else 14
            dst = 15
            rows = pl.ds(start, half) if way == RIGHT else pl.ds(start + half, keep - half)
        else:
            src = 0 if step == 0 else (2 * step - 1 if way == RIGHT else 2 * step)
            dst = 2 * step + 1 if way == RIGHT else 2 * step + 2
            rows = pl.ds(start, keep)
        return pltpu.make_async_remote_copy(
            src_ref=W[c].at[src, rows], dst_ref=W[c].at[dst, rows],
            send_sem=ssem.at[c, way, step], recv_sem=rsem.at[c, way, step],
            device_id={"fs": right if way == RIGHT else left}, device_id_type=pl.DeviceIdType.MESH,
        )

    def lend_copy(c, pos):
        _, _, start, lent = cut(c)
        start = pl.multiple_of((W[c].shape[1] - lent) - start, 16)
        return pltpu.make_async_remote_copy(
            src_ref=W[c].at[pos, pl.ds(start, lent)], dst_ref=W[c].at[pos, pl.ds(start, lent)],
            send_sem=ysend.at[c, pos], recv_sem=yrecv.at[c, pos],
            device_id={"grp": mate}, device_id_type=pl.DeviceIdType.MESH,
        )

    def hop(c, step):
        if step > 0:
            ring_copy(c, RIGHT, step - 1).wait_recv()
            ring_copy(c, LEFT, step - 1).wait_recv()
        if step < 8:
            for way in (RIGHT, LEFT):
                copy = ring_copy(c, way, step)
                copy.start()
                sends.append(copy)
        if PAIRED and step > 0:
            for pos in steps_positions(step):
                copy = lend_copy(c, pos)
                copy.start()
                sends.append(copy)

    def arrived(c, step):
        if PAIRED and step > 0:
            for pos in steps_positions(step):
                _, _, start, lent = cut(c)
                rows = pl.ds(start, lent)
                pltpu.make_async_remote_copy(
                    src_ref=W[c].at[pos, rows], dst_ref=W[c].at[pos, rows],
                    send_sem=ysend.at[c, pos], recv_sem=yrecv.at[c, pos],
                    device_id={"grp": mate}, device_id_type=pl.DeviceIdType.MESH,
                ).wait_recv()

    def spread(kind, src_of, dst, lo, hi):
        for d in range(1, 16):
            peer = lax.rem(tp + d, ntp)
            copy = pltpu.make_async_remote_copy(
                src_ref=src_of(peer), dst_ref=dst.at[tp, lo:hi],
                send_sem=xsend.at[kind, d], recv_sem=xrecv.at[kind, d],
                device_id={"tp": peer}, device_id_type=pl.DeviceIdType.MESH,
            )
            copy.start()
            sends.append(copy)

    def collect(kind, dst, lo, hi):
        for d in range(1, 16):
            peer = lax.rem(tp + ntp - d, ntp)
            part = dst.at[peer, lo:hi]
            pltpu.make_async_remote_copy(
                src_ref=part, dst_ref=part, send_sem=xsend.at[kind, d], recv_sem=xrecv.at[kind, d],
                device_id={"tp": peer}, device_id_type=pl.DeviceIdType.MESH,
            ).wait_recv()

    def sum_terms(t, r, lo, hi):
        total = t[tp, lo:hi].astype(jnp.float32)
        for d in range(1, 16):
            total = total + r[lax.rem(tp + d, ntp), lo:hi].astype(jnp.float32)
        return total

    def norm_first():
        squares = jnp.zeros((tok.shape[0], wide), jnp.float32)
        for pos in range(16):
            b = block_of(pos)
            v = tok[:, pl.ds(pl.multiple_of(b * wide, wide), wide)].astype(jnp.float32)
            xf[pos] = v
            squares = squares + v * v
        scale = lax.rsqrt(jnp.sum(squares, axis=1, keepdims=True) / tok.shape[1] + EPS)
        for pos in range(16):
            x1[pos] = (xf[pos] * scale * gain1[pl.ds(block_of(pos), 1), :]).astype(jnp.bfloat16)

    def gate_task(second, positions):
        gw, uw = (w3, w4) if second else (w0, w1)
        gates = values = None
        for pos in positions:
            if second:
                rows = x2[:, pos].astype(jnp.float32).reshape(tok.shape[0], wide).astype(jnp.bfloat16)
            else:
                rows = x1[pos]
            a, b = nt(rows, gw[pos]), nt(rows, uw[pos])
            gates, values = (a, b) if gates is None else (gates + a, values + b)
        if 0 in positions:
            acc[0], acc[1] = gates, values
        else:
            acc[0] += gates
            acc[1] += values

    def hidden_task():
        g = acc[0]
        hid[...] = (g / (1.0 + jnp.exp(-g)) * acc[1]).astype(jnp.bfloat16)

    def down_task(second, positions):
        for pos in positions:
            if second:
                term = 0.5 * jnp.dot(hid[...], w5[pos], preferred_element_type=jnp.float32)
            else:
                term = 0.5 * jnp.dot(hid[...], w2[pos, 0:hidden_rows], preferred_element_type=jnp.float32)
                term = term + jnp.dot(mix[...], w2[pos, hidden_rows : w2.shape[1]], preferred_element_type=jnp.float32)
            (t2 if second else t1)[:, pos] = term.reshape(ntp, share, wide).astype(jnp.bfloat16)

    def resid_task():
        collect(0, r1, 0, 16)
        rows = pl.ds(pl.multiple_of(tp * share, share), share)
        total = sum_terms(t1, r1, 0, 16)
        value = xf[:, rows, :] + total
        resid[...] = value
        squares = jnp.sum(jnp.sum(value * value, axis=0), axis=-1, keepdims=True)
        scale = lax.rsqrt(squares / tok.shape[1] + EPS)
        for pos in range(16):
            nrm[pos] = (resid[pos] * scale * gain2[pl.ds(block_of(pos), 1), :]).astype(jnp.bfloat16)
        x2[tp] = nrm[...]
        spread(1, lambda peer: nrm, x2, 0, 16)

    def finish_sum(i, lo, hi):
        collect(2 + i, r2, lo, hi)
        value = (resid[lo:hi] + sum_terms(t2, r2, lo, hi)).astype(jnp.bfloat16)
        fin[lo:hi] = value
        done[tp, lo:hi] = value
        spread(5 + i, lambda peer: fin.at[lo:hi], done, lo, hi)

    def finish_join(i, lo, hi):
        collect(5 + i, done, lo, hi)
        for pos in range(lo, hi):
            rows = done[:, pos].astype(jnp.float32).reshape(tok.shape[0], wide).astype(jnp.bfloat16)
            out[:, pl.ds(pl.multiple_of(block_of(pos) * wide, wide), wide)] = rows

    lag = 1 if PAIRED else 0
    state = {"g1": 0, "d1": 0, "g2": 0, "d2": 0, "rs": None, "ag": None, "x2": False, "group": 0}

    def ready(chains, key, t):
        steps = []
        while state[key] <= 8 and all(state[key] + (lag if state[key] else 0) <= t - OFFSETS[c] for c in chains):
            steps.append(state[key])
            state[key] += 1
        return steps

    def run_down(second, chains, key, t):
        positions = []
        for s in ready(chains, key, t):
            for c in chains:
                arrived(c, s)
            positions += steps_positions(s)
        if positions:
            down_task(second, positions)

    def tasks(t):
        if t == 0:
            norm_first()
        for s in ready((0, 1), "g1", t):
            arrived(0, s)
            arrived(1, s)
            gate_task(False, steps_positions(s))
            if s == 8:
                hidden_task()
        if state["g1"] == 9:
            run_down(False, (2,), "d1", t)
        if state["d1"] == 9 and state["rs"] is None:
            spread(0, lambda peer: t1.at[peer], r1, 0, 16)
            state["rs"] = t
        if state["rs"] is not None and state["ag"] is None and t >= state["rs"] + SUM_AFTER:
            resid_task()
            state["ag"] = t
        if state["ag"] is not None and t >= state["ag"] + JOIN_AFTER:
            if not state["x2"]:
                collect(1, x2, 0, 16)
                state["x2"] = True
            for s in ready((3, 4), "g2", t):
                arrived(3, s)
                arrived(4, s)
                gate_task(True, steps_positions(s))
                if s == 8:
                    hidden_task()
            if state["g2"] == 9:
                run_down(True, (5,), "d2", t)
        here = 1 + 2 * (state["d2"] - 1) if state["d2"] else 0
        here = 16 if state["d2"] == 9 else here
        while state["group"] < len(GROUPS) and GROUPS[state["group"]][1] <= here:
            i = state["group"]
            lo, hi = GROUPS[i]
            spread(2 + i, lambda peer: t2.at[peer, lo:hi], r2, lo, hi)
            state["group"] += 1

    for t in range(SLOTS + 12):
        for c in range(6):
            step = t - OFFSETS[c]
            if 0 <= step <= 8:
                hop(c, step)
        tasks(t)
    for i, (lo, hi) in enumerate(GROUPS):
        finish_sum(i, lo, hi)
    for i, (lo, hi) in enumerate(GROUPS):
        finish_join(i, lo, hi)
    for copy in sends:
        copy.wait_send()


def local(tok, mix, n1, g1, u1, d1, ow, n2, g2, u2, d2):
    ntp, nfs = lax.axis_size("tp"), lax.axis_size("fs")
    rows, width = tok.shape
    share, wide, hidden_rows, heads = rows // ntp, width // nfs, g1.shape[1], mix.shape[1]
    bf, f32 = jnp.bfloat16, jnp.float32
    vmem = pl.BlockSpec(memory_space=pltpu.VMEM)
    hbm = pl.BlockSpec(memory_space=pl.ANY)
    block = pltpu.VMEM((nfs, hidden_rows, wide), bf)
    per_peer = pltpu.VMEM((ntp, nfs, share, wide), bf)
    own = pltpu.VMEM((nfs, share, wide), bf)
    kinds = 2 + 2 * len(GROUPS)
    return pl.pallas_call(
        body,
        out_shape=jax.ShapeDtypeStruct((rows, width), bf),
        in_specs=[vmem, vmem, vmem, vmem, vmem, vmem, hbm, hbm, vmem, vmem, hbm],
        out_specs=vmem,
        scratch_shapes=[
            block, block, pltpu.VMEM((nfs, hidden_rows + heads, wide), bf), block, block, block,
            pltpu.VMEM((nfs, rows, wide), f32),
            pltpu.VMEM((nfs, rows, wide), bf),
            pltpu.VMEM((2, rows, hidden_rows), f32),
            pltpu.VMEM((rows, hidden_rows), bf),
            per_peer, per_peer, per_peer, per_peer, own, per_peer, own, per_peer,
            pltpu.VMEM((nfs, share, wide), f32),
            pltpu.SemaphoreType.DMA((3,)),
            pltpu.SemaphoreType.DMA((6, 2, 8)),
            pltpu.SemaphoreType.DMA((6, 2, 8)),
            pltpu.SemaphoreType.DMA((6, 16)),
            pltpu.SemaphoreType.DMA((6, 16)),
            pltpu.SemaphoreType.DMA((kinds, 16)),
            pltpu.SemaphoreType.DMA((kinds, 16)),
        ],
        compiler_params=pltpu.CompilerParams(
            collective_id=0, has_side_effects=True, vmem_limit_bytes=48 << 20
        ),
    )(tok, mix, n1.reshape(nfs, wide), n2.reshape(nfs, wide), g1, u1, d1, ow, g2, u2, d2)


def solution(mesh):
    in_specs = (
        P(("grp", "fs"), None),
        P(("grp", "fs"), "tp"),
        P(),
        P("fs", "tp"),
        P("fs", "tp"),
        P("tp", "fs"),
        P("tp", "fs"),
        P(),
        P("fs", "tp"),
        P("fs", "tp"),
        P("tp", "fs"),
    )
    out_specs = P(("grp", "fs"), None)
    return jax.shard_map(local, mesh=mesh, in_specs=in_specs, out_specs=out_specs, check_vma=False)
```

```python
import functools

import jax
import jax.numpy as jnp
from jax import lax
from jax.experimental import pallas as pl
from jax.experimental.pallas import tpu as pltpu
from jax.sharding import PartitionSpec as P

EPS = 0.1
PAIRED = True
RIGHT, LEFT = 0, 1
FIRST, SECOND = (0, 1, 2), (3, 4, 5)
OFFSETS = (0, 0, 0, 6, 6, 6)
SLOTS = 15
SUM_AFTER = 3
JOIN_AFTER = 3
GROUPS = ((0, 9), (9, 13), (13, 16))


def steps_positions(step):
    if step == 0:
        return (0,)
    return (15,) if step == 8 else (2 * step - 1, 2 * step)


def nt(a, b):
    return lax.dot_general(a, b, (((1,), (1,)), ((), ())), preferred_element_type=jnp.float32)


def body(
    tok_in, mix_in, gain1_in, gain2_in, g1, u1, d1, ow, g2, u2, d2,
    out,
    tok, mix, gain1, gain2,
    w0, w1, w2, w3, w4, w5, xf, x1, acc, hid, t1, r1, t2, r2, nrm, x2, fin, done, resid,
    wsem, ssem, rsem, ysend, yrecv, xsend, xrecv,
):
    W = (w0, w1, w2, w3, w4, w5)
    z, tp, gr = lax.axis_index("fs"), lax.axis_index("tp"), lax.axis_index("grp")
    nz, ntp = lax.axis_size("fs"), lax.axis_size("tp")
    right, left = lax.rem(z + 1, nz), lax.rem(z + nz - 1, nz)
    parity = lax.rem(gr, 2)
    mate = gr + 1 - 2 * parity
    share = tok.shape[0] // ntp
    wide = tok.shape[1] // nz
    hidden_rows = g1.shape[0]

    def block_of(pos):
        if pos == 0:
            return z
        if pos == 15:
            return lax.rem(z + 8, nz)
        step = (pos + 1) // 2
        return lax.rem(z + nz - step, nz) if pos % 2 else lax.rem(z + step, nz)

    def cut(c):
        rows = W[c].shape[1]
        lent = rows // 3 // 16 * 16
        if not PAIRED:
            return 0, rows, 0, 0
        return pl.multiple_of(parity * lent, 16), rows - lent, pl.multiple_of((1 - parity) * (rows - lent), 16), lent

    barrier = pltpu.get_barrier_semaphore()
    pl.semaphore_signal(barrier, device_id={"fs": right}, device_id_type=pl.DeviceIdType.MESH)
    pl.semaphore_signal(barrier, device_id={"fs": left}, device_id_type=pl.DeviceIdType.MESH)
    for d in range(1, 16):
        pl.semaphore_signal(barrier, device_id={"tp": lax.rem(tp + d, ntp)}, device_id_type=pl.DeviceIdType.MESH)
    if PAIRED:
        pl.semaphore_signal(barrier, device_id={"grp": mate}, device_id_type=pl.DeviceIdType.MESH)

    sources = (
        (g1, w0.at[0]), (u1, w1.at[0]), (d1, w2.at[0, 0:hidden_rows]), (ow, w2.at[0, hidden_rows : w2.shape[1]]),
        (tok_in, tok), (gain1_in, gain1), (mix_in, mix), (gain2_in, gain2), (g2, w3.at[0]), (u2, w4.at[0]), (d2, w5.at[0]),
    )
    loads = [pltpu.make_async_copy(src, dst, wsem.at[i]) for i, (src, dst) in enumerate(sources)]
    for load in loads:
        load.start()
    for load in loads[:4]:
        load.wait()
    pl.semaphore_wait(barrier, 18 if PAIRED else 17)

    sends = []

    def ring_copy(c, way, step):
        start, keep, _, _ = cut(c)
        if step == 7:
            half = keep // 32 * 16
            src = 13 if way == RIGHT else 14
            dst = 15
            rows = pl.ds(start, half) if way == RIGHT else pl.ds(start + half, keep - half)
        else:
            src = 0 if step == 0 else (2 * step - 1 if way == RIGHT else 2 * step)
            dst = 2 * step + 1 if way == RIGHT else 2 * step + 2
            rows = pl.ds(start, keep)
        return pltpu.make_async_remote_copy(
            src_ref=W[c].at[src, rows], dst_ref=W[c].at[dst, rows],
            send_sem=ssem.at[c, way, step], recv_sem=rsem.at[c, way, step],
            device_id={"fs": right if way == RIGHT else left}, device_id_type=pl.DeviceIdType.MESH,
        )

    def lend_copy(c, pos):
        _, _, start, lent = cut(c)
        start = pl.multiple_of((W[c].shape[1] - lent) - start, 16)
        return pltpu.make_async_remote_copy(
            src_ref=W[c].at[pos, pl.ds(start, lent)], dst_ref=W[c].at[pos, pl.ds(start, lent)],
            send_sem=ysend.at[c, pos], recv_sem=yrecv.at[c, pos],
            device_id={"grp": mate}, device_id_type=pl.DeviceIdType.MESH,
        )

    def hop(c, step):
        if step > 0:
            ring_copy(c, RIGHT, step - 1).wait_recv()
            ring_copy(c, LEFT, step - 1).wait_recv()
        if step < 8:
            for way in (RIGHT, LEFT):
                copy = ring_copy(c, way, step)
                copy.start()
                sends.append(copy)
        if PAIRED and step > 0:
            for pos in steps_positions(step):
                copy = lend_copy(c, pos)
                copy.start()
                sends.append(copy)

    def arrived(c, step):
        if PAIRED and step > 0:
            for pos in steps_positions(step):
                _, _, start, lent = cut(c)
                rows = pl.ds(start, lent)
                pltpu.make_async_remote_copy(
                    src_ref=W[c].at[pos, rows], dst_ref=W[c].at[pos, rows],
                    send_sem=ysend.at[c, pos], recv_sem=yrecv.at[c, pos],
                    device_id={"grp": mate}, device_id_type=pl.DeviceIdType.MESH,
                ).wait_recv()

    def spread(kind, src_of, dst, lo, hi):
        for d in range(1, 16):
            peer = lax.rem(tp + d, ntp)
            copy = pltpu.make_async_remote_copy(
                src_ref=src_of(peer), dst_ref=dst.at[tp, lo:hi],
                send_sem=xsend.at[kind, d], recv_sem=xrecv.at[kind, d],
                device_id={"tp": peer}, device_id_type=pl.DeviceIdType.MESH,
            )
            copy.start()
            sends.append(copy)

    def collect(kind, dst, lo, hi):
        for d in range(1, 16):
            peer = lax.rem(tp + ntp - d, ntp)
            part = dst.at[peer, lo:hi]
            pltpu.make_async_remote_copy(
                src_ref=part, dst_ref=part, send_sem=xsend.at[kind, d], recv_sem=xrecv.at[kind, d],
                device_id={"tp": peer}, device_id_type=pl.DeviceIdType.MESH,
            ).wait_recv()

    def sum_terms(t, r, lo, hi):
        total = t[tp, lo:hi].astype(jnp.float32)
        for d in range(1, 16):
            total = total + r[lax.rem(tp + d, ntp), lo:hi].astype(jnp.float32)
        return total

    def norm_first():
        squares = jnp.zeros((tok.shape[0], wide), jnp.float32)
        for pos in range(16):
            b = block_of(pos)
            v = tok[:, pl.ds(pl.multiple_of(b * wide, wide), wide)].astype(jnp.float32)
            xf[pos] = v
            squares = squares + v * v
        scale = lax.rsqrt(jnp.sum(squares, axis=1, keepdims=True) / tok.shape[1] + EPS)
        for pos in range(16):
            x1[pos] = (xf[pos] * scale * gain1[pl.ds(block_of(pos), 1), :]).astype(jnp.bfloat16)

    def gate_task(second, positions):
        gw, uw = (w3, w4) if second else (w0, w1)
        gates = values = None
        for pos in positions:
            if second:
                rows = x2[:, pos].astype(jnp.float32).reshape(tok.shape[0], wide).astype(jnp.bfloat16)
            else:
                rows = x1[pos]
            a, b = nt(rows, gw[pos]), nt(rows, uw[pos])
            gates, values = (a, b) if gates is None else (gates + a, values + b)
        if 0 in positions:
            acc[0], acc[1] = gates, values
        else:
            acc[0] += gates
            acc[1] += values

    def hidden_task():
        g = acc[0]
        hid[...] = (g / (1.0 + jnp.exp(-g)) * acc[1]).astype(jnp.bfloat16)

    def down_task(second, positions):
        for pos in positions:
            if second:
                term = 0.5 * jnp.dot(hid[...], w5[pos], preferred_element_type=jnp.float32)
            else:
                term = 0.5 * jnp.dot(hid[...], w2[pos, 0:hidden_rows], preferred_element_type=jnp.float32)
                term = term + jnp.dot(mix[...], w2[pos, hidden_rows : w2.shape[1]], preferred_element_type=jnp.float32)
            (t2 if second else t1)[:, pos] = term.reshape(ntp, share, wide).astype(jnp.bfloat16)

    def resid_task():
        collect(0, r1, 0, 16)
        rows = pl.ds(pl.multiple_of(tp * share, share), share)
        total = sum_terms(t1, r1, 0, 16)
        value = xf[:, rows, :] + total
        resid[...] = value
        squares = jnp.sum(jnp.sum(value * value, axis=0), axis=-1, keepdims=True)
        scale = lax.rsqrt(squares / tok.shape[1] + EPS)
        for pos in range(16):
            nrm[pos] = (resid[pos] * scale * gain2[pl.ds(block_of(pos), 1), :]).astype(jnp.bfloat16)
        x2[tp] = nrm[...]
        spread(1, lambda peer: nrm, x2, 0, 16)

    def finish_sum(i, lo, hi):
        collect(2 + i, r2, lo, hi)
        value = (resid[lo:hi] + sum_terms(t2, r2, lo, hi)).astype(jnp.bfloat16)
        fin[lo:hi] = value
        done[tp, lo:hi] = value
        spread(5 + i, lambda peer: fin.at[lo:hi], done, lo, hi)

    def finish_join(i, lo, hi):
        collect(5 + i, done, lo, hi)
        for pos in range(lo, hi):
            rows = done[:, pos].astype(jnp.float32).reshape(tok.shape[0], wide).astype(jnp.bfloat16)
            out[:, pl.ds(pl.multiple_of(block_of(pos) * wide, wide), wide)] = rows

    lag = 1 if PAIRED else 0
    state = {"g1": 0, "d1": 0, "g2": 0, "d2": 0, "rs": None, "ag": None, "x2": False, "group": 0}

    def ready(chains, key, t):
        steps = []
        while state[key] <= 8 and all(state[key] + (lag if state[key] else 0) <= t - OFFSETS[c] for c in chains):
            steps.append(state[key])
            state[key] += 1
        return steps

    def run_down(second, chains, key, t):
        positions = []
        for s in ready(chains, key, t):
            for c in chains:
                arrived(c, s)
            positions += steps_positions(s)
        if positions:
            down_task(second, positions)

    def tasks(t):
        if t == 0:
            for load in loads[4:]:
                load.wait()
            norm_first()
        for s in ready((0, 1), "g1", t):
            arrived(0, s)
            arrived(1, s)
            gate_task(False, steps_positions(s))
            if s == 8:
                hidden_task()
        if state["g1"] == 9:
            run_down(False, (2,), "d1", t)
        if state["d1"] == 9 and state["rs"] is None:
            spread(0, lambda peer: t1.at[peer], r1, 0, 16)
            state["rs"] = t
        if state["rs"] is not None and state["ag"] is None and t >= state["rs"] + SUM_AFTER:
            resid_task()
            state["ag"] = t
        if state["ag"] is not None and t >= state["ag"] + JOIN_AFTER:
            if not state["x2"]:
                collect(1, x2, 0, 16)
                state["x2"] = True
            for s in ready((3, 4), "g2", t):
                arrived(3, s)
                arrived(4, s)
                gate_task(True, steps_positions(s))
                if s == 8:
                    hidden_task()
            if state["g2"] == 9:
                run_down(True, (5,), "d2", t)
        here = 1 + 2 * (state["d2"] - 1) if state["d2"] else 0
        here = 16 if state["d2"] == 9 else here
        while state["group"] < len(GROUPS) and GROUPS[state["group"]][1] <= here:
            i = state["group"]
            lo, hi = GROUPS[i]
            spread(2 + i, lambda peer: t2.at[peer, lo:hi], r2, lo, hi)
            state["group"] += 1

    for t in range(SLOTS + 12):
        for c in range(6):
            step = t - OFFSETS[c]
            if 0 <= step <= 8:
                hop(c, step)
        tasks(t)
    for i, (lo, hi) in enumerate(GROUPS):
        finish_sum(i, lo, hi)
    for i, (lo, hi) in enumerate(GROUPS):
        finish_join(i, lo, hi)
    for copy in sends:
        copy.wait_send()


def local(tok, mix, n1, g1, u1, d1, ow, n2, g2, u2, d2):
    ntp, nfs = lax.axis_size("tp"), lax.axis_size("fs")
    rows, width = tok.shape
    share, wide, hidden_rows, heads = rows // ntp, width // nfs, g1.shape[1], mix.shape[1]
    bf, f32 = jnp.bfloat16, jnp.float32
    vmem = pl.BlockSpec(memory_space=pltpu.VMEM)
    hbm = pl.BlockSpec(memory_space=pltpu.HBM)
    block = pltpu.VMEM((nfs, hidden_rows, wide), bf)
    per_peer = pltpu.VMEM((ntp, nfs, share, wide), bf)
    own = pltpu.VMEM((nfs, share, wide), bf)
    kinds = 2 + 2 * len(GROUPS)
    return pl.pallas_call(
        body,
        out_shape=jax.ShapeDtypeStruct((rows, width), bf),
        in_specs=[hbm] * 11,
        out_specs=vmem,
        scratch_shapes=[
            pltpu.VMEM((rows, width), bf), pltpu.VMEM((rows, heads), bf),
            pltpu.VMEM((nfs, wide), f32), pltpu.VMEM((nfs, wide), f32),
            block, block, pltpu.VMEM((nfs, hidden_rows + heads, wide), bf), block, block, block,
            pltpu.VMEM((nfs, rows, wide), f32),
            pltpu.VMEM((nfs, rows, wide), bf),
            pltpu.VMEM((2, rows, hidden_rows), f32),
            pltpu.VMEM((rows, hidden_rows), bf),
            per_peer, per_peer, per_peer, per_peer, own, per_peer, own, per_peer,
            pltpu.VMEM((nfs, share, wide), f32),
            pltpu.SemaphoreType.DMA((11,)),
            pltpu.SemaphoreType.DMA((6, 2, 8)),
            pltpu.SemaphoreType.DMA((6, 2, 8)),
            pltpu.SemaphoreType.DMA((6, 16)),
            pltpu.SemaphoreType.DMA((6, 16)),
            pltpu.SemaphoreType.DMA((kinds, 16)),
            pltpu.SemaphoreType.DMA((kinds, 16)),
        ],
        compiler_params=pltpu.CompilerParams(
            collective_id=0, has_side_effects=True, vmem_limit_bytes=67043328
        ),
    )(tok, mix, n1.reshape(nfs, wide), n2.reshape(nfs, wide), g1.T, u1.T, d1, ow, g2.T, u2.T, d2)


def solution(mesh):
    in_specs = (
        P(("grp", "fs"), None),
        P(("grp", "fs"), "tp"),
        P(),
        P("fs", "tp"),
        P("fs", "tp"),
        P("tp", "fs"),
        P("tp", "fs"),
        P(),
        P("fs", "tp"),
        P("fs", "tp"),
        P("tp", "fs"),
    )
    out_specs = P(("grp", "fs"), None)
    return jax.shard_map(local, mesh=mesh, in_specs=in_specs, out_specs=out_specs, check_vma=False)
```

```python
import functools

import jax
import jax.numpy as jnp
from jax import lax
from jax.experimental import pallas as pl
from jax.experimental.pallas import tpu as pltpu
from jax.sharding import PartitionSpec as P

EPS = 0.1
PAIRED = True
RIGHT, LEFT = 0, 1
OFFSETS = (0, 0, 0, 6, 6, 6)
SUM_AFTER = 2
JOIN_AFTER = 2
GROUPS = ((0, 7), (7, 16))


def schedule(offsets=OFFSETS, sum_after=SUM_AFTER, join_after=JOIN_AFTER, groups=GROUPS, lag=1):
    events, at = [], {"g1": 0, "d1": 0, "g2": 0, "d2": 0}
    sent = joined = None
    summed, group, spare = None, 0, []

    def ready(chains, key, t):
        steps = []
        while at[key] <= 8 and all(at[key] + (lag if at[key] else 0) <= t - offsets[c] for c in chains):
            steps.append(at[key])
            at[key] += 1
        return steps

    for t in range(40):
        for c in range(6):
            if 0 <= t - offsets[c] <= 8:
                events.append(("hop", c, t - offsets[c]))
        if t == 0:
            events.append(("norm",))
        for step in ready((0, 1), "g1", t):
            events.append(("gate", 0, step))
            if step == 8:
                events.append(("hidden",))
        if at["g1"] == 9:
            for step in ready((2,), "d1", t):
                events.append(("down", 0, step))
        if at["d1"] == 9 and sent is None:
            events += [("pair", 0, 0, 16), ("spread", 0, 0, 16)]
            sent = t
        if sent is not None and summed is None and t >= sent + sum_after:
            events.append(("resid",))
            summed = t
        if summed is not None and t >= summed + join_after:
            if joined is None:
                events += [("forward", 1, 0, 16), ("join", 1, 0, 16)]
                joined = t
            for step in ready((3, 4), "g2", t):
                events.append(("gate", 1, step))
                if step == 8:
                    events.append(("hidden",))
            if at["g2"] == 9:
                for step in ready((5,), "d2", t):
                    events.append(("down", 1, step))
                    here = 16 if step == 8 else 2 * step + 1
                    while group < len(groups) and groups[group][1] <= here:
                        events.append(("pair", 2 + 2 * group) + groups[group])
                        group += 1
    for name, first in (("spread", 2), ("finish", 2), ("forward", 3), ("out", 3)):
        for i, (lo, hi) in enumerate(groups):
            events.append((name, first + 2 * i, lo, hi))
    return events


def steps_positions(step):
    if step == 0:
        return (0,)
    return (15,) if step == 8 else (2 * step - 1, 2 * step)


def nt(a, b):
    return lax.dot_general(a, b, (((1,), (1,)), ((), ())), preferred_element_type=jnp.float32)


def body(
    tok_in, mix_in, gain1_in, gain2_in, g1, u1, d1, ow, g2, u2, d2,
    out,
    tok, mix, gain1, gain2,
    w0, w1, w2, w3, w4, w5, xf, x1, acc, hid, t1, q1, s1, r1, t2, q2, s2, r2, nrm, x2, fin, done, resid,
    wsem, ssem, rsem, ysend, yrecv, xsend, xrecv,
):
    W = (w0, w1, w2, w3, w4, w5)
    z, tp, gr = lax.axis_index("fs"), lax.axis_index("tp"), lax.axis_index("grp")
    nz, ntp = lax.axis_size("fs"), lax.axis_size("tp")
    right, left = lax.rem(z + 1, nz), lax.rem(z + nz - 1, nz)
    parity = lax.rem(gr, 2)
    mate = gr + 1 - 2 * parity
    chips = ntp // 2
    chip, core = tp // 2, lax.rem(tp, 2)
    partner = tp + 1 - 2 * core
    share = tok.shape[0] // ntp
    wide = tok.shape[1] // nz
    hidden_rows = g1.shape[0]

    def block_of(pos):
        if pos == 0:
            return z
        if pos == 15:
            return lax.rem(z + 8, nz)
        step = (pos + 1) // 2
        return lax.rem(z + nz - step, nz) if pos % 2 else lax.rem(z + step, nz)

    def cut(c):
        rows = W[c].shape[1]
        lent = rows // 3 // 16 * 16
        if not PAIRED:
            return 0, rows, 0, 0
        return pl.multiple_of(parity * lent, 16), rows - lent, pl.multiple_of((1 - parity) * (rows - lent), 16), lent

    barrier = pltpu.get_barrier_semaphore()
    pl.semaphore_signal(barrier, device_id={"fs": right}, device_id_type=pl.DeviceIdType.MESH)
    pl.semaphore_signal(barrier, device_id={"fs": left}, device_id_type=pl.DeviceIdType.MESH)
    for d in range(1, chips):
        pl.semaphore_signal(barrier, device_id={"tp": lax.rem(tp + 2 * d, ntp)}, device_id_type=pl.DeviceIdType.MESH)
    pl.semaphore_signal(barrier, device_id={"tp": partner}, device_id_type=pl.DeviceIdType.MESH)
    if PAIRED:
        pl.semaphore_signal(barrier, device_id={"grp": mate}, device_id_type=pl.DeviceIdType.MESH)

    sources = (
        (g1, w0.at[0]), (u1, w1.at[0]), (d1, w2.at[0, 0:hidden_rows]), (ow, w2.at[0, hidden_rows : w2.shape[1]]),
        (tok_in, tok), (gain1_in, gain1), (mix_in, mix), (gain2_in, gain2), (g2, w3.at[0]), (u2, w4.at[0]), (d2, w5.at[0]),
    )
    loads = [pltpu.make_async_copy(src, dst, wsem.at[i]) for i, (src, dst) in enumerate(sources)]
    for load in loads:
        load.start()
    for load in loads[:4]:
        load.wait()
    pl.semaphore_wait(barrier, chips + (3 if PAIRED else 2))

    sends = []

    def start(copy):
        copy.start()
        sends.append(copy)

    def ring_copy(c, way, step):
        start, keep, _, _ = cut(c)
        if step == 7:
            half = keep // 32 * 16
            src = 13 if way == RIGHT else 14
            dst = 15
            rows = pl.ds(start, half) if way == RIGHT else pl.ds(start + half, keep - half)
        else:
            src = 0 if step == 0 else (2 * step - 1 if way == RIGHT else 2 * step)
            dst = 2 * step + 1 if way == RIGHT else 2 * step + 2
            rows = pl.ds(start, keep)
        return pltpu.make_async_remote_copy(
            src_ref=W[c].at[src, rows], dst_ref=W[c].at[dst, rows],
            send_sem=ssem.at[c, way, step], recv_sem=rsem.at[c, way, step],
            device_id={"fs": right if way == RIGHT else left}, device_id_type=pl.DeviceIdType.MESH,
        )

    def lend_copy(c, pos):
        _, _, start, lent = cut(c)
        start = pl.multiple_of((W[c].shape[1] - lent) - start, 16)
        return pltpu.make_async_remote_copy(
            src_ref=W[c].at[pos, pl.ds(start, lent)], dst_ref=W[c].at[pos, pl.ds(start, lent)],
            send_sem=ysend.at[c, pos], recv_sem=yrecv.at[c, pos],
            device_id={"grp": mate}, device_id_type=pl.DeviceIdType.MESH,
        )

    def hop(c, step):
        for way in (RIGHT, LEFT):
            if step > 0:
                ring_copy(c, way, step - 1).wait_recv()
            if step < 8:
                start(ring_copy(c, way, step))
            if PAIRED and 0 < step < 8:
                start(lend_copy(c, 2 * step - 1 if way == RIGHT else 2 * step))
        if PAIRED and step == 8:
            start(lend_copy(c, 15))

    def arrived(c, step):
        if PAIRED and step > 0:
            for pos in steps_positions(step):
                _, _, start, lent = cut(c)
                rows = pl.ds(start, lent)
                pltpu.make_async_remote_copy(
                    src_ref=W[c].at[pos, rows], dst_ref=W[c].at[pos, rows],
                    send_sem=ysend.at[c, pos], recv_sem=yrecv.at[c, pos],
                    device_id={"grp": mate}, device_id_type=pl.DeviceIdType.MESH,
                ).wait_recv()

    def to_peer(kind, i, src, dst, peer):
        return pltpu.make_async_remote_copy(
            src_ref=src, dst_ref=dst, send_sem=xsend.at[kind, i], recv_sem=xrecv.at[kind, i],
            device_id={"tp": peer}, device_id_type=pl.DeviceIdType.MESH,
        )

    def terms(kind):
        return (t1, q1, s1, r1) if kind == 0 else (t2, q2, s2, r2)

    def pair_send(kind, lo, hi):
        t, q, _, _ = terms(kind)
        start(to_peer(kind, 0, t.at[1 - core, :, lo:hi], q.at[:, lo:hi], partner))

    def spread(kind, lo, hi):
        t, q, s, r = terms(kind)
        to_peer(kind, 0, q.at[:, lo:hi], q.at[:, lo:hi], partner).wait_recv()
        s[:, lo:hi] = (t[core, :, lo:hi].astype(jnp.float32) + q[:, lo:hi].astype(jnp.float32)).astype(jnp.bfloat16)
        for d in range(1, chips):
            there = lax.rem(chip + d, chips)
            start(to_peer(kind, d, s.at[there, lo:hi], r.at[chip, lo:hi], lax.rem(tp + 2 * d, ntp)))

    def collect(kind, lo, hi):
        t, q, _, r = terms(kind)
        total = t[core, chip, lo:hi].astype(jnp.float32) + q[chip, lo:hi].astype(jnp.float32)
        for d in range(1, chips):
            part = r.at[lax.rem(chip + chips - d, chips), lo:hi]
            to_peer(kind, d, part, part, partner).wait_recv()
        for d in range(1, chips):
            total = total + r[lax.rem(chip + d, chips), lo:hi].astype(jnp.float32)
        return total

    def share_rows(kind, own, dst, lo, hi):
        for d in range(1, chips):
            start(to_peer(kind, d, own.at[lo:hi], dst.at[chip, core, lo:hi], lax.rem(tp + 2 * d, ntp)))
        start(to_peer(kind, 0, own.at[lo:hi], dst.at[chip, core, lo:hi], partner))

    def forward(kind, dst, lo, hi):
        for d in sorted(range(1, chips), key=lambda d: min(d, chips - d)):
            part = dst.at[lax.rem(chip + chips - d, chips), core, lo:hi]
            to_peer(kind, d, part, part, partner).wait_recv()
            start(to_peer(kind, chips + d, part, part, partner))

    def join(kind, dst, lo, hi):
        for d in range(chips):
            part = dst.at[lax.rem(chip + chips - d, chips), 1 - core, lo:hi]
            to_peer(kind, chips + d if d else 0, part, part, partner).wait_recv()

    def rows_of(ref, pos):
        return ref[:, :, pos].astype(jnp.float32).reshape(tok.shape[0], wide).astype(jnp.bfloat16)

    def norm_first():
        squares = jnp.zeros((tok.shape[0], wide), jnp.float32)
        for pos in range(16):
            b = block_of(pos)
            v = tok[:, pl.ds(pl.multiple_of(b * wide, wide), wide)].astype(jnp.float32)
            xf[pos] = v
            squares = squares + v * v
        scale = lax.rsqrt(jnp.sum(squares, axis=1, keepdims=True) / tok.shape[1] + EPS)
        for pos in range(16):
            x1[pos] = (xf[pos] * scale * gain1[pl.ds(block_of(pos), 1), :]).astype(jnp.bfloat16)

    def gate_task(second, positions):
        gw, uw = (w3, w4) if second else (w0, w1)
        gates = values = None
        for pos in positions:
            if second:
                rows = rows_of(x2, pos)
            else:
                rows = x1[pos]
            a, b = nt(rows, gw[pos]), nt(rows, uw[pos])
            gates, values = (a, b) if gates is None else (gates + a, values + b)
        if 0 in positions:
            acc[0], acc[1] = gates, values
        else:
            acc[0] += gates
            acc[1] += values

    def hidden_task():
        g = acc[0]
        hid[...] = (g / (1.0 + jnp.exp(-g)) * acc[1]).astype(jnp.bfloat16)

    def down_task(second, positions):
        for pos in positions:
            if second:
                term = 0.5 * jnp.dot(hid[...], w5[pos], preferred_element_type=jnp.float32)
            else:
                term = 0.5 * jnp.dot(hid[...], w2[pos, 0:hidden_rows], preferred_element_type=jnp.float32)
                term = term + jnp.dot(mix[...], w2[pos, hidden_rows : w2.shape[1]], preferred_element_type=jnp.float32)
            term = term.reshape(chips, 2, share, wide).astype(jnp.bfloat16)
            for c in range(2):
                (t2 if second else t1)[c, :, pos] = term[:, c]

    def resid_task():
        total = collect(0, 0, 16)
        rows = pl.ds(pl.multiple_of(tp * share, share), share)
        value = xf[:, rows, :] + total
        resid[...] = value
        squares = jnp.sum(jnp.sum(value * value, axis=0), axis=-1, keepdims=True)
        scale = lax.rsqrt(squares / tok.shape[1] + EPS)
        for pos in range(16):
            nrm[pos] = (resid[pos] * scale * gain2[pl.ds(block_of(pos), 1), :]).astype(jnp.bfloat16)
        share_rows(1, nrm, x2, 0, 16)
        x2[chip, core] = nrm[...]

    for event in schedule(lag=1 if PAIRED else 0):
        name, args = event[0], event[1:]
        if name == "hop":
            if args == (3, 0):
                for load in loads[8:]:
                    load.wait()
            hop(*args)
        elif name == "norm":
            for load in loads[4:8]:
                load.wait()
            norm_first()
        elif name == "gate":
            second, step = args
            for c in (3, 4) if second else (0, 1):
                arrived(c, step)
            gate_task(second, steps_positions(step))
        elif name == "hidden":
            hidden_task()
        elif name == "down":
            second, step = args
            arrived(5 if second else 2, step)
            down_task(second, steps_positions(step))
        elif name == "pair":
            pair_send(*args)
        elif name == "spread":
            spread(*args)
        elif name == "resid":
            resid_task()
        elif name == "finish":
            kind, lo, hi = args
            fin[lo:hi] = (resid[lo:hi] + collect(kind, lo, hi)).astype(jnp.bfloat16)
            share_rows(kind + 1, fin, done, lo, hi)
            done[chip, core, lo:hi] = fin[lo:hi]
        elif name == "forward":
            forward(args[0], x2 if args[0] == 1 else done, *args[1:])
        elif name == "join":
            join(args[0], x2, *args[1:])
        elif name == "out":
            kind, lo, hi = args
            join(kind, done, lo, hi)
            for pos in range(lo, hi):
                out[:, pl.ds(pl.multiple_of(block_of(pos) * wide, wide), wide)] = rows_of(done, pos)
    for copy in sends:
        copy.wait_send()


def local(tok, mix, n1, g1, u1, d1, ow, n2, g2, u2, d2):
    ntp, nfs = lax.axis_size("tp"), lax.axis_size("fs")
    rows, width = tok.shape
    share, wide, hidden_rows, heads = rows // ntp, width // nfs, g1.shape[1], mix.shape[1]
    chips = ntp // 2
    bf, f32 = jnp.bfloat16, jnp.float32
    vmem = pl.BlockSpec(memory_space=pltpu.VMEM)
    hbm = pl.BlockSpec(memory_space=pltpu.HBM)
    block = pltpu.VMEM((nfs, hidden_rows, wide), bf)
    both = pltpu.VMEM((2, chips, nfs, share, wide), bf)
    joined = pltpu.VMEM((chips, 2, nfs, share, wide), bf)
    half = pltpu.VMEM((chips, nfs, share, wide), bf)
    own = pltpu.VMEM((nfs, share, wide), bf)
    kinds = 2 + 2 * len(GROUPS)
    return pl.pallas_call(
        body,
        out_shape=jax.ShapeDtypeStruct((rows, width), bf),
        in_specs=[hbm] * 11,
        out_specs=vmem,
        scratch_shapes=[
            pltpu.VMEM((rows, width), bf), pltpu.VMEM((rows, heads), bf),
            pltpu.VMEM((nfs, wide), f32), pltpu.VMEM((nfs, wide), f32),
            block, block, pltpu.VMEM((nfs, hidden_rows + heads, wide), bf), block, block, block,
            pltpu.VMEM((nfs, rows, wide), f32),
            pltpu.VMEM((nfs, rows, wide), bf),
            pltpu.VMEM((2, rows, hidden_rows), f32),
            pltpu.VMEM((rows, hidden_rows), bf),
            both, half, half, half, both, half, half, half, own, joined, own, joined,
            pltpu.VMEM((nfs, share, wide), f32),
            pltpu.SemaphoreType.DMA((11,)),
            pltpu.SemaphoreType.DMA((6, 2, 8)),
            pltpu.SemaphoreType.DMA((6, 2, 8)),
            pltpu.SemaphoreType.DMA((6, 16)),
            pltpu.SemaphoreType.DMA((6, 16)),
            pltpu.SemaphoreType.DMA((kinds, 16)),
            pltpu.SemaphoreType.DMA((kinds, 16)),
        ],
        compiler_params=pltpu.CompilerParams(
            collective_id=0, has_side_effects=True, vmem_limit_bytes=67043328
        ),
    )(tok, mix, n1.reshape(nfs, wide), n2.reshape(nfs, wide), g1.T, u1.T, d1, ow, g2.T, u2.T, d2)


def solution(mesh):
    in_specs = (
        P(("grp", "fs"), None),
        P(("grp", "fs"), "tp"),
        P(),
        P("fs", "tp"),
        P("fs", "tp"),
        P("tp", "fs"),
        P("tp", "fs"),
        P(),
        P("fs", "tp"),
        P("fs", "tp"),
        P("tp", "fs"),
    )
    out_specs = P(("grp", "fs"), None)
    return jax.shard_map(local, mesh=mesh, in_specs=in_specs, out_specs=out_specs, check_vma=False)
```

```python
import functools

import jax
import jax.numpy as jnp
from jax import lax
from jax.experimental import pallas as pl
from jax.experimental.pallas import tpu as pltpu
from jax.sharding import PartitionSpec as P

EPS = 0.1
PAIRED = True
RIGHT, LEFT = 0, 1
SCALES = 2
EVENTS = (
    ("hop", 0, 0, 0), ("hop", 0, 0, 1), ("hop", 1, 0, 0), ("hop", 1, 0, 1), ("hop", 2, 0, 0), ("hop", 2, 0, 1),
    ("hop", 0, 1, 0), ("hop", 0, 1, 1), ("hop", 1, 1, 0), ("hop", 1, 1, 1), ("hop", 2, 1, 0), ("hop", 2, 1, 1),
    ("hop", 0, 2, 0), ("hop", 0, 2, 1), ("hop", 1, 2, 0), ("hop", 1, 2, 1), ("norm",), ("hop", 2, 2, 0),
    ("hop", 2, 2, 1), ("hop", 0, 3, 0), ("hop", 0, 3, 1), ("hop", 1, 3, 0), ("hop", 1, 3, 1), ("hop", 2, 3, 0),
    ("gate", 0, 0), ("hop", 2, 3, 1), ("hop", 0, 4, 0), ("hop", 0, 4, 1), ("hop", 1, 4, 0), ("hop", 1, 4, 1),
    ("hop", 2, 4, 0), ("hop", 2, 4, 1), ("hop", 0, 5, 0), ("hop", 0, 5, 1), ("hop", 1, 5, 0), ("hop", 1, 5, 1),
    ("hop", 2, 5, 0), ("hop", 2, 5, 1), ("hop", 0, 6, 0), ("hop", 0, 6, 1), ("hop", 1, 6, 0), ("hop", 1, 6, 1),
    ("gate", 0, 5), ("hop", 2, 6, 0), ("hop", 2, 6, 1), ("gate", 0, 1), ("hop", 3, 0, 0), ("hop", 3, 0, 1),
    ("hop", 4, 0, 0), ("hop", 4, 0, 1), ("hop", 0, 7, 0), ("hop", 0, 7, 1), ("hop", 1, 7, 0), ("hop", 1, 7, 1),
    ("gate", 0, 6), ("hop", 2, 7, 0), ("hop", 2, 7, 1), ("hop", 3, 1, 0), ("hop", 3, 1, 1), ("gate", 0, 2),
    ("hop", 4, 1, 0), ("gate", 0, 4), ("hop", 4, 1, 1), ("hop", 5, 0, 0), ("gate", 0, 3), ("hop", 5, 0, 1),
    ("hop", 0, 8, 0), ("hop", 0, 8, 1), ("hop", 1, 8, 0), ("hop", 1, 8, 1), ("hop", 2, 8, 0), ("hop", 2, 8, 1),
    ("hop", 3, 2, 0), ("hop", 3, 2, 1), ("hop", 4, 2, 0), ("gate", 0, 7), ("hop", 4, 2, 1), ("gate", 0, 8),
    ("hidden", 0), ("down", 0, 5), ("hop", 5, 1, 0), ("hop", 5, 1, 1), ("down", 0, 2), ("down", 0, 3),
    ("down", 0, 1), ("down", 0, 8), ("hop", 3, 3, 0), ("down", 0, 4), ("hop", 3, 3, 1), ("down", 0, 0),
    ("down", 0, 7), ("down", 0, 6), ("hop", 4, 3, 0), ("hop", 4, 3, 1), ("pair", 0, 0, 16), ("hop", 5, 2, 0),
    ("hop", 5, 2, 1), ("spread", 0, 0, 16), ("hop", 3, 4, 0), ("hop", 3, 4, 1), ("hop", 4, 4, 0), ("hop", 4, 4, 1),
    ("hop", 5, 3, 0), ("hop", 5, 3, 1), ("hop", 3, 5, 0), ("hop", 3, 5, 1), ("hop", 4, 5, 0), ("hop", 4, 5, 1),
    ("hop", 5, 4, 0), ("hop", 5, 4, 1), ("collect", 0, 0, 16), ("hop", 3, 6, 0), ("hop", 3, 6, 1), ("hop", 4, 6, 0),
    ("hop", 4, 6, 1), ("hop", 5, 5, 0), ("hop", 5, 5, 1), ("scale", 2), ("hop", 3, 7, 0), ("hop", 3, 7, 1),
    ("hop", 4, 7, 0), ("hop", 4, 7, 1), ("forward", 1, 0, 16), ("hop", 5, 6, 0), ("hop", 5, 6, 1), ("hop", 3, 8, 0),
    ("join", 1, 0, 16), ("gate", 1, 0), ("hop", 3, 8, 1), ("forward", 2, 0, 1), ("gate", 1, 1), ("hop", 4, 8, 0),
    ("hop", 4, 8, 1), ("gate", 1, 7), ("gate", 1, 6), ("gate", 1, 2), ("hop", 5, 7, 0), ("hop", 5, 7, 1),
    ("gate", 1, 5), ("gate", 1, 3), ("gate", 1, 8), ("gate", 1, 4), ("join", 2, 0, 1), ("hidden", 1), ("down", 1, 1),
    ("hop", 5, 8, 0), ("hop", 5, 8, 1), ("down", 1, 3), ("down", 1, 4), ("down", 1, 6), ("down", 1, 5),
    ("down", 1, 0), ("down", 1, 7), ("down", 1, 2), ("pair", 3, 0, 9), ("down", 1, 8), ("pair", 5, 9, 16),
    ("spread", 3, 0, 9), ("spread", 5, 9, 16), ("finish", 3, 0, 9), ("finish", 5, 9, 16), ("forward", 4, 0, 9),
    ("forward", 6, 9, 16), ("out", 4, 0, 9), ("out", 6, 9, 16),
)


def steps_positions(step):
    if step == 0:
        return (0,)
    return (15,) if step == 8 else (2 * step - 1, 2 * step)


def nt(a, b):
    return lax.dot_general(a, b, (((1,), (1,)), ((), ())), preferred_element_type=jnp.float32)


def body(
    tok_in, mix_in, gain1_in, gain2_in, g1, u1, d1, ow, g2, u2, d2,
    out,
    tok, mix, gain1, gain2,
    w0, w1, w2, w3, w4, w5, xf, x1, acc, hid, t1, q1, s1, r1, t2, q2, s2, r2, nrm, x2, fin, done, resid, squares, mine, scales,
    wsem, ssem, rsem, ysend, yrecv, xsend, xrecv,
):
    W = (w0, w1, w2, w3, w4, w5)
    z, tp, gr = lax.axis_index("fs"), lax.axis_index("tp"), lax.axis_index("grp")
    nz, ntp = lax.axis_size("fs"), lax.axis_size("tp")
    right, left = lax.rem(z + 1, nz), lax.rem(z + nz - 1, nz)
    parity = lax.rem(gr, 2)
    mate = gr + 1 - 2 * parity
    chips = ntp // 2
    chip, core = tp // 2, lax.rem(tp, 2)
    partner = tp + 1 - 2 * core
    share = tok.shape[0] // ntp
    wide = tok.shape[1] // nz
    hidden_rows = g1.shape[0]

    def block_of(pos):
        if pos == 0:
            return z
        if pos == 15:
            return lax.rem(z + 8, nz)
        step = (pos + 1) // 2
        return lax.rem(z + nz - step, nz) if pos % 2 else lax.rem(z + step, nz)

    def cut(c):
        rows = W[c].shape[1]
        lent = rows // 3 // 16 * 16
        if not PAIRED:
            return 0, rows, 0, 0
        return pl.multiple_of(parity * lent, 16), rows - lent, pl.multiple_of((1 - parity) * (rows - lent), 16), lent

    barrier = pltpu.get_barrier_semaphore()
    pl.semaphore_signal(barrier, device_id={"fs": right}, device_id_type=pl.DeviceIdType.MESH)
    pl.semaphore_signal(barrier, device_id={"fs": left}, device_id_type=pl.DeviceIdType.MESH)
    for d in range(1, chips):
        pl.semaphore_signal(barrier, device_id={"tp": lax.rem(tp + 2 * d, ntp)}, device_id_type=pl.DeviceIdType.MESH)
    pl.semaphore_signal(barrier, device_id={"tp": partner}, device_id_type=pl.DeviceIdType.MESH)
    if PAIRED:
        pl.semaphore_signal(barrier, device_id={"grp": mate}, device_id_type=pl.DeviceIdType.MESH)

    sources = (
        (g1, w0.at[0]), (u1, w1.at[0]), (d1, w2.at[0, 0:hidden_rows]), (ow, w2.at[0, hidden_rows : w2.shape[1]]),
        (tok_in, tok), (gain1_in, gain1), (mix_in, mix), (gain2_in, gain2), (g2, w3.at[0]), (u2, w4.at[0]), (d2, w5.at[0]),
    )
    loads = [pltpu.make_async_copy(src, dst, wsem.at[i]) for i, (src, dst) in enumerate(sources)]
    for load in loads:
        load.start()
    pl.semaphore_wait(barrier, chips + (3 if PAIRED else 2))

    sends = []

    def start(copy):
        copy.start()
        sends.append(copy)

    def ring_copy(c, way, step):
        start, keep, _, _ = cut(c)
        if step == 7:
            half = keep // 32 * 16
            src = 13 if way == RIGHT else 14
            dst = 15
            rows = pl.ds(start, half) if way == RIGHT else pl.ds(start + half, keep - half)
        else:
            src = 0 if step == 0 else (2 * step - 1 if way == RIGHT else 2 * step)
            dst = 2 * step + 1 if way == RIGHT else 2 * step + 2
            rows = pl.ds(start, keep)
        return pltpu.make_async_remote_copy(
            src_ref=W[c].at[src, rows], dst_ref=W[c].at[dst, rows],
            send_sem=ssem.at[c, way, step], recv_sem=rsem.at[c, way, step],
            device_id={"fs": right if way == RIGHT else left}, device_id_type=pl.DeviceIdType.MESH,
        )

    def lend_copy(c, pos):
        _, _, start, lent = cut(c)
        start = pl.multiple_of((W[c].shape[1] - lent) - start, 16)
        return pltpu.make_async_remote_copy(
            src_ref=W[c].at[pos, pl.ds(start, lent)], dst_ref=W[c].at[pos, pl.ds(start, lent)],
            send_sem=ysend.at[c, pos], recv_sem=yrecv.at[c, pos],
            device_id={"grp": mate}, device_id_type=pl.DeviceIdType.MESH,
        )

    def hop(c, step, way):
        if step > 0:
            ring_copy(c, way, step - 1).wait_recv()
        if step < 8:
            start(ring_copy(c, way, step))
        if PAIRED and 0 < step < 8:
            start(lend_copy(c, 2 * step - 1 if way == RIGHT else 2 * step))
        if PAIRED and step == 8 and way == LEFT:
            start(lend_copy(c, 15))

    def arrived(c, step):
        if PAIRED and step > 0:
            for pos in steps_positions(step):
                _, _, start, lent = cut(c)
                rows = pl.ds(start, lent)
                pltpu.make_async_remote_copy(
                    src_ref=W[c].at[pos, rows], dst_ref=W[c].at[pos, rows],
                    send_sem=ysend.at[c, pos], recv_sem=yrecv.at[c, pos],
                    device_id={"grp": mate}, device_id_type=pl.DeviceIdType.MESH,
                ).wait_recv()

    def to_peer(kind, i, src, dst, peer):
        return pltpu.make_async_remote_copy(
            src_ref=src, dst_ref=dst, send_sem=xsend.at[kind, i], recv_sem=xrecv.at[kind, i],
            device_id={"tp": peer}, device_id_type=pl.DeviceIdType.MESH,
        )

    far_first = sorted(range(1, chips), key=lambda d: -min(d, chips - d))

    def terms(kind):
        return (t1, q1, s1, r1) if kind < SCALES else (t2, q2, s2, r2)

    def pair_send(kind, lo, hi):
        t, q, _, _ = terms(kind)
        start(to_peer(kind, 0, t.at[1 - core, :, lo:hi], q.at[:, lo:hi], partner))

    def spread(kind, lo, hi):
        t, q, s, r = terms(kind)
        to_peer(kind, 0, q.at[:, lo:hi], q.at[:, lo:hi], partner).wait_recv()
        s[:, lo:hi] = (t[core, :, lo:hi].astype(jnp.float32) + q[:, lo:hi].astype(jnp.float32)).astype(jnp.bfloat16)
        for d in far_first:
            there = lax.rem(chip + d, chips)
            start(to_peer(kind, d, s.at[there, lo:hi], r.at[chip, lo:hi], lax.rem(tp + 2 * d, ntp)))

    def collect(kind, lo, hi):
        t, q, _, r = terms(kind)
        total = t[core, chip, lo:hi].astype(jnp.float32) + q[chip, lo:hi].astype(jnp.float32)
        for d in range(1, chips):
            part = r.at[lax.rem(chip + chips - d, chips), lo:hi]
            to_peer(kind, d, part, part, partner).wait_recv()
        for d in range(1, chips):
            total = total + r[lax.rem(chip + d, chips), lo:hi].astype(jnp.float32)
        return total

    def share_rows(kind, own, dst, lo, hi):
        for d in far_first:
            start(to_peer(kind, d, own.at[lo:hi], dst.at[chip, core, lo:hi], lax.rem(tp + 2 * d, ntp)))
        start(to_peer(kind, 0, own.at[lo:hi], dst.at[chip, core, lo:hi], partner))

    def forward(kind, dst, lo, hi):
        for d in far_first:
            part = dst.at[lax.rem(chip + chips - d, chips), core, lo:hi]
            to_peer(kind, d, part, part, partner).wait_recv()
            start(to_peer(kind, chips + d, part, part, partner))

    def join(kind, dst, lo, hi):
        for d in range(chips):
            part = dst.at[lax.rem(chip + chips - d, chips), 1 - core, lo:hi]
            to_peer(kind, chips + d if d else 0, part, part, partner).wait_recv()

    def rows_of(ref, pos):
        return ref[:, :, pos].astype(jnp.float32).reshape(tok.shape[0], wide).astype(jnp.bfloat16)

    def norm_first():
        squares = jnp.zeros((tok.shape[0], wide), jnp.float32)
        for pos in range(16):
            b = block_of(pos)
            v = tok[:, pl.ds(pl.multiple_of(b * wide, wide), wide)].astype(jnp.float32)
            xf[pos] = v
            squares = squares + v * v
        scale = lax.rsqrt(jnp.sum(squares, axis=1, keepdims=True) / tok.shape[1] + EPS)
        for pos in range(16):
            x1[pos] = (xf[pos] * scale * gain1[pl.ds(block_of(pos), 1), :]).astype(jnp.bfloat16)

    def gate_task(second, positions):
        gw, uw = (w3, w4) if second else (w0, w1)
        gates = values = None
        for pos in positions:
            if second:
                rows = rows_of(x2, pos)
            else:
                rows = x1[pos]
            a, b = nt(rows, gw[pos]), nt(rows, uw[pos])
            gates, values = (a, b) if gates is None else (gates + a, values + b)
        if 0 in positions:
            acc[0], acc[1] = gates, values
        else:
            acc[0] += gates
            acc[1] += values

    def hidden_task(second):
        g, v = acc[0], acc[1]
        if second:
            scale = scales[:, :, 0].reshape(tok.shape[0], wide)[:, 0:1]
            g, v = g * scale, v * scale
        hid[...] = (g / (1.0 + jnp.exp(-g)) * v).astype(jnp.bfloat16)

    def down_task(second, positions):
        for pos in positions:
            if second:
                term = 0.5 * jnp.dot(hid[...], w5[pos], preferred_element_type=jnp.float32)
            else:
                term = 0.5 * jnp.dot(hid[...], w2[pos, 0:hidden_rows], preferred_element_type=jnp.float32)
                term = term + jnp.dot(mix[...], w2[pos, hidden_rows : w2.shape[1]], preferred_element_type=jnp.float32)
            term = term.reshape(chips, 2, share, wide).astype(jnp.bfloat16)
            for c in range(2):
                (t2 if second else t1)[c, :, pos] = term[:, c]

    def collect_task(kind, lo, hi):
        rows = pl.ds(pl.multiple_of(tp * share, share), share)
        value = xf[lo:hi, rows, :] + collect(kind, lo, hi)
        resid[lo:hi] = value
        here = jnp.sum(value * value, axis=0)
        squares[...] = here if kind == 0 else squares[...] + here
        for pos in range(lo, hi):
            nrm[pos] = (resid[pos] * gain2[pl.ds(block_of(pos), 1), :]).astype(jnp.bfloat16)
        x2[chip, core, lo:hi] = nrm[lo:hi]
        share_rows(kind + 1, nrm, x2, lo, hi)

    def scale_task(kind):
        total = jnp.sum(squares[...], axis=-1, keepdims=True)
        scale = jnp.broadcast_to(lax.rsqrt(total / tok.shape[1] + EPS), squares.shape)
        mine[0] = scale
        scales[chip, core, 0] = scale
        share_rows(kind, mine, scales, 0, 1)

    def landing(kind):
        return x2 if kind < SCALES else (scales if kind == SCALES else done)

    def finish_task(kind, lo, hi):
        fin[lo:hi] = (resid[lo:hi] + collect(kind, lo, hi)).astype(jnp.bfloat16)
        share_rows(kind + 1, fin, done, lo, hi)
        done[chip, core, lo:hi] = fin[lo:hi]

    def out_task(kind, lo, hi):
        join(kind, done, lo, hi)
        for pos in range(lo, hi):
            out[:, pl.ds(pl.multiple_of(block_of(pos) * wide, wide), wide)] = rows_of(done, pos)

    waited = set()

    def need(*numbers):
        for i in numbers:
            if i not in waited:
                loads[i].wait()
                waited.add(i)

    own_loads = ((0,), (1,), (2, 3), (8,), (9,), (10,))
    for name, *args in EVENTS:
        if name == "hop":
            if args[1] == 0:
                need(*own_loads[args[0]])
            hop(*args)
        elif name == "norm":
            need(4, 5, 6, 7)
            norm_first()
        elif name == "gate":
            for c in (3, 4) if args[0] else (0, 1):
                arrived(c, args[1])
            gate_task(args[0], steps_positions(args[1]))
        elif name == "hidden":
            hidden_task(args[0])
        elif name == "down":
            arrived(5 if args[0] else 2, args[1])
            down_task(args[0], steps_positions(args[1]))
        elif name == "pair":
            pair_send(*args)
        elif name == "spread":
            spread(*args)
        elif name == "collect":
            collect_task(*args)
        elif name == "scale":
            scale_task(*args)
        elif name == "forward":
            forward(args[0], landing(args[0]), *args[1:])
        elif name == "join":
            join(args[0], landing(args[0]), *args[1:])
        elif name == "finish":
            finish_task(*args)
        else:
            out_task(*args)
    for copy in sends:
        copy.wait_send()


def local(tok, mix, n1, g1, u1, d1, ow, n2, g2, u2, d2):
    ntp, nfs = lax.axis_size("tp"), lax.axis_size("fs")
    rows, width = tok.shape
    share, wide, hidden_rows, heads = rows // ntp, width // nfs, g1.shape[1], mix.shape[1]
    chips = ntp // 2
    bf, f32 = jnp.bfloat16, jnp.float32
    vmem = pl.BlockSpec(memory_space=pltpu.VMEM)
    hbm = pl.BlockSpec(memory_space=pltpu.HBM)
    block = pltpu.VMEM((nfs, hidden_rows, wide), bf)
    both = pltpu.VMEM((2, chips, nfs, share, wide), bf)
    joined = pltpu.VMEM((chips, 2, nfs, share, wide), bf)
    half = pltpu.VMEM((chips, nfs, share, wide), bf)
    own = pltpu.VMEM((nfs, share, wide), bf)
    kinds = 1 + max(event[1] for event in EVENTS if event[0] == "out")
    return pl.pallas_call(
        body,
        out_shape=jax.ShapeDtypeStruct((rows, width), bf),
        in_specs=[hbm] * 11,
        out_specs=vmem,
        scratch_shapes=[
            pltpu.VMEM((rows, width), bf), pltpu.VMEM((rows, heads), bf),
            pltpu.VMEM((nfs, wide), f32), pltpu.VMEM((nfs, wide), f32),
            block, block, pltpu.VMEM((nfs, hidden_rows + heads, wide), bf), block, block, block,
            pltpu.VMEM((nfs, rows, wide), f32),
            pltpu.VMEM((nfs, rows, wide), bf),
            pltpu.VMEM((2, rows, hidden_rows), f32),
            pltpu.VMEM((rows, hidden_rows), bf),
            both, half, half, half, both, half, half, half, own, joined, own, joined,
            pltpu.VMEM((nfs, share, wide), f32), pltpu.VMEM((share, wide), f32),
            pltpu.VMEM((1, share, wide), f32), pltpu.VMEM((chips, 2, 1, share, wide), f32),
            pltpu.SemaphoreType.DMA((11,)),
            pltpu.SemaphoreType.DMA((6, 2, 8)),
            pltpu.SemaphoreType.DMA((6, 2, 8)),
            pltpu.SemaphoreType.DMA((6, 16)),
            pltpu.SemaphoreType.DMA((6, 16)),
            pltpu.SemaphoreType.DMA((kinds, 16)),
            pltpu.SemaphoreType.DMA((kinds, 16)),
        ],
        compiler_params=pltpu.CompilerParams(
            collective_id=0, has_side_effects=True, vmem_limit_bytes=67043328
        ),
    )(tok, mix, n1.reshape(nfs, wide), n2.reshape(nfs, wide), g1.T, u1.T, d1, ow, g2.T, u2.T, d2)


def solution(mesh):
    in_specs = (
        P(("grp", "fs"), None),
        P(("grp", "fs"), "tp"),
        P(),
        P("fs", "tp"),
        P("fs", "tp"),
        P("tp", "fs"),
        P("tp", "fs"),
        P(),
        P("fs", "tp"),
        P("fs", "tp"),
        P("tp", "fs"),
    )
    out_specs = P(("grp", "fs"), None)
    return jax.shard_map(local, mesh=mesh, in_specs=in_specs, out_specs=out_specs, check_vma=False)
```

```python
import functools

import jax
import jax.numpy as jnp
from jax import lax
from jax.experimental import pallas as pl
from jax.experimental.pallas import tpu as pltpu
from jax.sharding import PartitionSpec as P

EPS = 0.1
PAIRED = True
RIGHT, LEFT = 0, 1
SCALES = 2
EVENTS = (
    ("hop", 0, 0, 0), ("hop", 0, 0, 1), ("hop", 1, 0, 0), ("hop", 1, 0, 1), ("hop", 2, 0, 0), ("hop", 2, 0, 1),
    ("hop", 0, 1, 0), ("hop", 0, 1, 1), ("hop", 1, 1, 0), ("hop", 1, 1, 1), ("hop", 2, 1, 0), ("hop", 2, 1, 1),
    ("hop", 0, 2, 0), ("hop", 0, 2, 1), ("hop", 1, 2, 0), ("hop", 1, 2, 1), ("norm",), ("hop", 2, 2, 0),
    ("hop", 2, 2, 1), ("hop", 0, 3, 0), ("hop", 0, 3, 1), ("hop", 1, 3, 0), ("hop", 1, 3, 1), ("hop", 2, 3, 0),
    ("gate", 0, 0), ("hop", 2, 3, 1), ("hop", 0, 4, 0), ("hop", 0, 4, 1), ("hop", 1, 4, 0), ("hop", 1, 4, 1),
    ("hop", 2, 4, 0), ("hop", 2, 4, 1), ("hop", 0, 5, 0), ("hop", 0, 5, 1), ("hop", 1, 5, 0), ("hop", 1, 5, 1),
    ("hop", 2, 5, 0), ("hop", 2, 5, 1), ("hop", 0, 6, 0), ("hop", 0, 6, 1), ("hop", 1, 6, 0), ("hop", 1, 6, 1),
    ("gate", 0, 5), ("hop", 2, 6, 0), ("hop", 2, 6, 1), ("gate", 0, 1), ("hop", 3, 0, 0), ("hop", 3, 0, 1),
    ("hop", 4, 0, 0), ("hop", 4, 0, 1), ("hop", 0, 7, 0), ("hop", 0, 7, 1), ("hop", 1, 7, 0), ("hop", 1, 7, 1),
    ("gate", 0, 6), ("hop", 2, 7, 0), ("hop", 2, 7, 1), ("hop", 3, 1, 0), ("hop", 3, 1, 1), ("gate", 0, 2),
    ("hop", 4, 1, 0), ("gate", 0, 4), ("hop", 4, 1, 1), ("hop", 5, 0, 0), ("gate", 0, 3), ("hop", 5, 0, 1),
    ("hop", 0, 8, 0), ("hop", 0, 8, 1), ("hop", 1, 8, 0), ("hop", 1, 8, 1), ("hop", 2, 8, 0), ("hop", 2, 8, 1),
    ("hop", 3, 2, 0), ("hop", 3, 2, 1), ("hop", 4, 2, 0), ("gate", 0, 7), ("hop", 4, 2, 1), ("gate", 0, 8),
    ("hidden", 0), ("down", 0, 5), ("hop", 5, 1, 0), ("hop", 5, 1, 1), ("down", 0, 2), ("down", 0, 3),
    ("down", 0, 1), ("down", 0, 8), ("hop", 3, 3, 0), ("down", 0, 4), ("hop", 3, 3, 1), ("down", 0, 0),
    ("down", 0, 7), ("down", 0, 6), ("hop", 4, 3, 0), ("hop", 4, 3, 1), ("pair", 0, 0, 16), ("hop", 5, 2, 0),
    ("hop", 5, 2, 1), ("spread", 0, 0, 16), ("hop", 3, 4, 0), ("hop", 3, 4, 1), ("hop", 4, 4, 0), ("hop", 4, 4, 1),
    ("hop", 5, 3, 0), ("hop", 5, 3, 1), ("hop", 3, 5, 0), ("hop", 3, 5, 1), ("hop", 4, 5, 0), ("hop", 4, 5, 1),
    ("hop", 5, 4, 0), ("hop", 5, 4, 1), ("collect", 0, 0, 16), ("hop", 3, 6, 0), ("hop", 3, 6, 1), ("hop", 4, 6, 0),
    ("hop", 4, 6, 1), ("hop", 5, 5, 0), ("hop", 5, 5, 1), ("scale", 2), ("hop", 3, 7, 0), ("hop", 3, 7, 1),
    ("hop", 4, 7, 0), ("hop", 4, 7, 1), ("forward", 1, 0, 16), ("hop", 5, 6, 0), ("hop", 5, 6, 1), ("hop", 3, 8, 0),
    ("join", 1, 0, 16), ("gate", 1, 0), ("hop", 3, 8, 1), ("forward", 2, 0, 1), ("gate", 1, 1), ("hop", 4, 8, 0),
    ("hop", 4, 8, 1), ("gate", 1, 7), ("gate", 1, 6), ("gate", 1, 2), ("hop", 5, 7, 0), ("hop", 5, 7, 1),
    ("gate", 1, 5), ("gate", 1, 3), ("gate", 1, 8), ("gate", 1, 4), ("join", 2, 0, 1), ("hidden", 1), ("down", 1, 1),
    ("hop", 5, 8, 0), ("hop", 5, 8, 1), ("down", 1, 3), ("down", 1, 4), ("down", 1, 6), ("down", 1, 5),
    ("down", 1, 0), ("down", 1, 7), ("down", 1, 2), ("pair", 3, 0, 9), ("down", 1, 8), ("pair", 5, 9, 16),
    ("spread", 3, 0, 9), ("spread", 5, 9, 16), ("finish", 3, 0, 9), ("finish", 5, 9, 16), ("forward", 4, 0, 9),
    ("forward", 6, 9, 16), ("out", 4, 0, 9), ("out", 6, 9, 16),
)


def steps_positions(step):
    if step == 0:
        return (0,)
    return (15,) if step == 8 else (2 * step - 1, 2 * step)


def nt(a, b):
    return lax.dot_general(a, b, (((1,), (1,)), ((), ())), preferred_element_type=jnp.float32)


def body(
    tok_in, mix_in, gain1_in, gain2_in, g1, u1, d1, ow, g2, u2, d2,
    out,
    tok, mix, gain1, gain2,
    w0, w1, w2, w3, w4, w5, xf, x1, acc, hid, t1, q1, s1, r1, t2, q2, s2, r2, nrm, x2, fin, done, resid, squares, mine, scales,
    wsem, ssem, rsem, ysend, yrecv, xsend, xrecv,
):
    W = (w0, w1, w2, w3, w4, w5)
    z, tp, gr = lax.axis_index("fs"), lax.axis_index("tp"), lax.axis_index("grp")
    nz, ntp = lax.axis_size("fs"), lax.axis_size("tp")
    right, left = lax.rem(z + 1, nz), lax.rem(z + nz - 1, nz)
    parity = lax.rem(gr, 2)
    mate = gr + 1 - 2 * parity
    chips = ntp // 2
    chip, core = tp // 2, lax.rem(tp, 2)
    partner = tp + 1 - 2 * core
    share = tok.shape[0] // ntp
    wide = tok.shape[1] // nz
    hidden_rows = g1.shape[0]

    def block_of(pos):
        if pos == 0:
            return z
        if pos == 15:
            return lax.rem(z + 8, nz)
        step = (pos + 1) // 2
        return lax.rem(z + nz - step, nz) if pos % 2 else lax.rem(z + step, nz)

    def cut(c):
        rows = W[c].shape[1]
        lent = (rows - 1) // 3 // 16 * 16
        if not PAIRED:
            return 0, rows, 0, 0
        return pl.multiple_of(parity * lent, 16), rows - lent, pl.multiple_of((1 - parity) * (rows - lent), 16), lent

    barrier = pltpu.get_barrier_semaphore()
    pl.semaphore_signal(barrier, device_id={"fs": right}, device_id_type=pl.DeviceIdType.MESH)
    pl.semaphore_signal(barrier, device_id={"fs": left}, device_id_type=pl.DeviceIdType.MESH)
    for d in range(1, chips):
        pl.semaphore_signal(barrier, device_id={"tp": lax.rem(tp + 2 * d, ntp)}, device_id_type=pl.DeviceIdType.MESH)
    pl.semaphore_signal(barrier, device_id={"tp": partner}, device_id_type=pl.DeviceIdType.MESH)
    if PAIRED:
        pl.semaphore_signal(barrier, device_id={"grp": mate}, device_id_type=pl.DeviceIdType.MESH)

    sources = (
        (g1, w0.at[0]), (u1, w1.at[0]), (d1, w2.at[0, 0:hidden_rows]), (ow, w2.at[0, hidden_rows : w2.shape[1]]),
        (tok_in, tok), (gain1_in, gain1), (mix_in, mix), (gain2_in, gain2), (g2, w3.at[0]), (u2, w4.at[0]), (d2, w5.at[0]),
    )
    loads = [pltpu.make_async_copy(src, dst, wsem.at[i]) for i, (src, dst) in enumerate(sources)]
    for load in loads:
        load.start()
    pl.semaphore_wait(barrier, chips + (3 if PAIRED else 2))

    sends = []

    def start(copy):
        copy.start()
        sends.append(copy)

    def ring_copy(c, way, step):
        start, keep, _, _ = cut(c)
        if step == 7:
            half = keep // 32 * 16
            src = 13 if way == RIGHT else 14
            dst = 15
            rows = pl.ds(start, half) if way == RIGHT else pl.ds(start + half, keep - half)
        else:
            src = 0 if step == 0 else (2 * step - 1 if way == RIGHT else 2 * step)
            dst = 2 * step + 1 if way == RIGHT else 2 * step + 2
            rows = pl.ds(start, keep)
        return pltpu.make_async_remote_copy(
            src_ref=W[c].at[src, rows], dst_ref=W[c].at[dst, rows],
            send_sem=ssem.at[c, way, step], recv_sem=rsem.at[c, way, step],
            device_id={"fs": right if way == RIGHT else left}, device_id_type=pl.DeviceIdType.MESH,
        )

    def lend_copy(c, pos):
        _, _, start, lent = cut(c)
        start = pl.multiple_of((W[c].shape[1] - lent) - start, 16)
        return pltpu.make_async_remote_copy(
            src_ref=W[c].at[pos, pl.ds(start, lent)], dst_ref=W[c].at[pos, pl.ds(start, lent)],
            send_sem=ysend.at[c, pos], recv_sem=yrecv.at[c, pos],
            device_id={"grp": mate}, device_id_type=pl.DeviceIdType.MESH,
        )

    def hop(c, step, way):
        if step > 0:
            ring_copy(c, way, step - 1).wait_recv()
        if step < 8:
            start(ring_copy(c, way, step))
        if PAIRED and 0 < step < 8:
            start(lend_copy(c, 2 * step - 1 if way == RIGHT else 2 * step))
        if PAIRED and step == 8 and way == LEFT:
            start(lend_copy(c, 15))

    def arrived(c, step):
        if PAIRED and step > 0:
            for pos in steps_positions(step):
                _, _, start, lent = cut(c)
                rows = pl.ds(start, lent)
                pltpu.make_async_remote_copy(
                    src_ref=W[c].at[pos, rows], dst_ref=W[c].at[pos, rows],
                    send_sem=ysend.at[c, pos], recv_sem=yrecv.at[c, pos],
                    device_id={"grp": mate}, device_id_type=pl.DeviceIdType.MESH,
                ).wait_recv()

    def to_peer(kind, i, src, dst, peer):
        return pltpu.make_async_remote_copy(
            src_ref=src, dst_ref=dst, send_sem=xsend.at[kind, i], recv_sem=xrecv.at[kind, i],
            device_id={"tp": peer}, device_id_type=pl.DeviceIdType.MESH,
        )

    far_first = sorted(range(1, chips), key=lambda d: -min(d, chips - d))

    def terms(kind):
        return (t1, q1, s1, r1) if kind < SCALES else (t2, q2, s2, r2)

    def pair_send(kind, lo, hi):
        t, q, _, _ = terms(kind)
        start(to_peer(kind, 0, t.at[1 - core, :, lo:hi], q.at[:, lo:hi], partner))

    def spread(kind, lo, hi):
        t, q, s, r = terms(kind)
        to_peer(kind, 0, q.at[:, lo:hi], q.at[:, lo:hi], partner).wait_recv()
        s[:, lo:hi] = (t[core, :, lo:hi].astype(jnp.float32) + q[:, lo:hi].astype(jnp.float32)).astype(jnp.bfloat16)
        for d in far_first:
            there = lax.rem(chip + d, chips)
            start(to_peer(kind, d, s.at[there, lo:hi], r.at[chip, lo:hi], lax.rem(tp + 2 * d, ntp)))

    def collect(kind, lo, hi):
        t, q, _, r = terms(kind)
        total = t[core, chip, lo:hi].astype(jnp.float32) + q[chip, lo:hi].astype(jnp.float32)
        for d in range(1, chips):
            part = r.at[lax.rem(chip + chips - d, chips), lo:hi]
            to_peer(kind, d, part, part, partner).wait_recv()
        for d in range(1, chips):
            total = total + r[lax.rem(chip + d, chips), lo:hi].astype(jnp.float32)
        return total

    def share_rows(kind, own, dst, lo, hi):
        for d in far_first:
            start(to_peer(kind, d, own.at[lo:hi], dst.at[chip, core, lo:hi], lax.rem(tp + 2 * d, ntp)))
        start(to_peer(kind, 0, own.at[lo:hi], dst.at[chip, core, lo:hi], partner))

    def forward(kind, dst, lo, hi):
        for d in far_first:
            part = dst.at[lax.rem(chip + chips - d, chips), core, lo:hi]
            to_peer(kind, d, part, part, partner).wait_recv()
            start(to_peer(kind, chips + d, part, part, partner))

    def join(kind, dst, lo, hi):
        for d in range(chips):
            part = dst.at[lax.rem(chip + chips - d, chips), 1 - core, lo:hi]
            to_peer(kind, chips + d if d else 0, part, part, partner).wait_recv()

    def rows_of(ref, pos):
        return ref[:, :, pos].astype(jnp.float32).reshape(tok.shape[0], wide).astype(jnp.bfloat16)

    def norm_first():
        squares = jnp.zeros((tok.shape[0], wide), jnp.float32)
        for pos in range(16):
            b = block_of(pos)
            v = tok[:, pl.ds(pl.multiple_of(b * wide, wide), wide)].astype(jnp.float32)
            xf[pos] = v
            squares = squares + v * v
        scale = lax.rsqrt(jnp.sum(squares, axis=1, keepdims=True) / tok.shape[1] + EPS)
        for pos in range(16):
            x1[pos] = (xf[pos] * scale * gain1[pl.ds(block_of(pos), 1), :]).astype(jnp.bfloat16)

    def gate_task(second, positions):
        gw, uw = (w3, w4) if second else (w0, w1)
        gates = values = None
        for pos in positions:
            if second:
                rows = rows_of(x2, pos)
            else:
                rows = x1[pos]
            a, b = nt(rows, gw[pos]), nt(rows, uw[pos])
            gates, values = (a, b) if gates is None else (gates + a, values + b)
        if 0 in positions:
            acc[0], acc[1] = gates, values
        else:
            acc[0] += gates
            acc[1] += values

    def hidden_task(second):
        g, v = acc[0], acc[1]
        if second:
            scale = scales[:, :, 0].reshape(tok.shape[0], wide)[:, 0:1]
            g, v = g * scale, v * scale
        hid[...] = (g / (1.0 + jnp.exp(-g)) * v).astype(jnp.bfloat16)

    def down_task(second, positions):
        for pos in positions:
            if second:
                term = 0.5 * jnp.dot(hid[...], w5[pos], preferred_element_type=jnp.float32)
            else:
                term = 0.5 * jnp.dot(hid[...], w2[pos, 0:hidden_rows], preferred_element_type=jnp.float32)
                term = term + jnp.dot(mix[...], w2[pos, hidden_rows : w2.shape[1]], preferred_element_type=jnp.float32)
            term = term.reshape(chips, 2, share, wide).astype(jnp.bfloat16)
            for c in range(2):
                (t2 if second else t1)[c, :, pos] = term[:, c]

    def collect_task(kind, lo, hi):
        rows = pl.ds(pl.multiple_of(tp * share, share), share)
        value = xf[lo:hi, rows, :] + collect(kind, lo, hi)
        resid[lo:hi] = value
        here = jnp.sum(value * value, axis=0)
        squares[...] = here if kind == 0 else squares[...] + here
        for pos in range(lo, hi):
            nrm[pos] = (resid[pos] * gain2[pl.ds(block_of(pos), 1), :]).astype(jnp.bfloat16)
        x2[chip, core, lo:hi] = nrm[lo:hi]
        share_rows(kind + 1, nrm, x2, lo, hi)

    def scale_task(kind):
        total = jnp.sum(squares[...], axis=-1, keepdims=True)
        scale = jnp.broadcast_to(lax.rsqrt(total / tok.shape[1] + EPS), squares.shape)
        mine[0] = scale
        scales[chip, core, 0] = scale
        share_rows(kind, mine, scales, 0, 1)

    def landing(kind):
        return x2 if kind < SCALES else (scales if kind == SCALES else done)

    def finish_task(kind, lo, hi):
        fin[lo:hi] = (resid[lo:hi] + collect(kind, lo, hi)).astype(jnp.bfloat16)
        share_rows(kind + 1, fin, done, lo, hi)
        done[chip, core, lo:hi] = fin[lo:hi]

    def out_task(kind, lo, hi):
        join(kind, done, lo, hi)
        for pos in range(lo, hi):
            out[:, pl.ds(pl.multiple_of(block_of(pos) * wide, wide), wide)] = rows_of(done, pos)

    waited = set()

    def need(*numbers):
        for i in numbers:
            if i not in waited:
                loads[i].wait()
                waited.add(i)

    own_loads = ((0,), (1,), (2, 3), (8,), (9,), (10,))
    for name, *args in EVENTS:
        if name == "hop":
            if args[1] == 0:
                need(*own_loads[args[0]])
            hop(*args)
        elif name == "norm":
            need(4, 5, 6, 7)
            norm_first()
        elif name == "gate":
            for c in (3, 4) if args[0] else (0, 1):
                arrived(c, args[1])
            gate_task(args[0], steps_positions(args[1]))
        elif name == "hidden":
            hidden_task(args[0])
        elif name == "down":
            arrived(5 if args[0] else 2, args[1])
            down_task(args[0], steps_positions(args[1]))
        elif name == "pair":
            pair_send(*args)
        elif name == "spread":
            spread(*args)
        elif name == "collect":
            collect_task(*args)
        elif name == "scale":
            scale_task(*args)
        elif name == "forward":
            forward(args[0], landing(args[0]), *args[1:])
        elif name == "join":
            join(args[0], landing(args[0]), *args[1:])
        elif name == "finish":
            finish_task(*args)
        else:
            out_task(*args)
    for copy in sends:
        copy.wait_send()


def local(tok, mix, n1, g1, u1, d1, ow, n2, g2, u2, d2):
    ntp, nfs = lax.axis_size("tp"), lax.axis_size("fs")
    rows, width = tok.shape
    share, wide, hidden_rows, heads = rows // ntp, width // nfs, g1.shape[1], mix.shape[1]
    chips = ntp // 2
    bf, f32 = jnp.bfloat16, jnp.float32
    vmem = pl.BlockSpec(memory_space=pltpu.VMEM)
    hbm = pl.BlockSpec(memory_space=pltpu.HBM)
    block = pltpu.VMEM((nfs, hidden_rows, wide), bf)
    both = pltpu.VMEM((2, chips, nfs, share, wide), bf)
    joined = pltpu.VMEM((chips, 2, nfs, share, wide), bf)
    half = pltpu.VMEM((chips, nfs, share, wide), bf)
    own = pltpu.VMEM((nfs, share, wide), bf)
    kinds = 1 + max(event[1] for event in EVENTS if event[0] == "out")
    return pl.pallas_call(
        body,
        out_shape=jax.ShapeDtypeStruct((rows, width), bf),
        in_specs=[hbm] * 11,
        out_specs=vmem,
        scratch_shapes=[
            pltpu.VMEM((rows, width), bf), pltpu.VMEM((rows, heads), bf),
            pltpu.VMEM((nfs, wide), f32), pltpu.VMEM((nfs, wide), f32),
            block, block, pltpu.VMEM((nfs, hidden_rows + heads, wide), bf), block, block, block,
            pltpu.VMEM((nfs, rows, wide), f32),
            pltpu.VMEM((nfs, rows, wide), bf),
            pltpu.VMEM((2, rows, hidden_rows), f32),
            pltpu.VMEM((rows, hidden_rows), bf),
            both, half, half, half, both, half, half, half, own, joined, own, joined,
            pltpu.VMEM((nfs, share, wide), f32), pltpu.VMEM((share, wide), f32),
            pltpu.VMEM((1, share, wide), f32), pltpu.VMEM((chips, 2, 1, share, wide), f32),
            pltpu.SemaphoreType.DMA((11,)),
            pltpu.SemaphoreType.DMA((6, 2, 8)),
            pltpu.SemaphoreType.DMA((6, 2, 8)),
            pltpu.SemaphoreType.DMA((6, 16)),
            pltpu.SemaphoreType.DMA((6, 16)),
            pltpu.SemaphoreType.DMA((kinds, 16)),
            pltpu.SemaphoreType.DMA((kinds, 16)),
        ],
        compiler_params=pltpu.CompilerParams(
            collective_id=0, has_side_effects=True, vmem_limit_bytes=67043328
        ),
    )(tok, mix, n1.reshape(nfs, wide), n2.reshape(nfs, wide), g1.T, u1.T, d1, ow, g2.T, u2.T, d2)


def solution(mesh):
    in_specs = (
        P(("grp", "fs"), None),
        P(("grp", "fs"), "tp"),
        P(),
        P("fs", "tp"),
        P("fs", "tp"),
        P("tp", "fs"),
        P("tp", "fs"),
        P(),
        P("fs", "tp"),
        P("fs", "tp"),
        P("tp", "fs"),
    )
    out_specs = P(("grp", "fs"), None)
    return jax.shard_map(local, mesh=mesh, in_specs=in_specs, out_specs=out_specs, check_vma=False)
```
